32 devices in a mesh: ep: 8 (over z, x), tp: 4 (over y, core).
Axes of the slice: x: 2, y: 2, z: 4, core: 2. Of those that a mesh axis runs over, the one named last changes fastest.
Arguments:
- tokens: bfloat16 [256, 4096], P('ep'), may hold values from -6 to 6
- mix_gain: bfloat16 [4096], replicated, may hold values from 0.099609375 to 1.8984375
- query_weight: bfloat16 [4096, 1024], P(None, 'tp'), may hold values from -0.09375 to 0.09375
- key_weight: bfloat16 [4096, 1024], P(None, 'tp'), may hold values from -0.09375 to 0.09375
- value_weight: bfloat16 [4096, 1024], P(None, 'tp'), may hold values from -0.09375 to 0.09375
- decay_weight: bfloat16 [4096, 8], replicated, may hold values from -0.09375 to 0.09375
- strength_weight: bfloat16 [4096, 8], replicated, may hold values from -0.09375 to 0.09375
- decay_rate: float32 [8], P('tp'), may hold values from 0.03 to 3
- head_gain: bfloat16 [128], replicated, may hold values from 0.099609375 to 1.8984375
- memory_state: float32 [256, 8, 128, 128], P('ep', 'tp'), may hold values from -0.6 to 0.6
- output_weight: bfloat16 [1024, 4096], P('tp'), may hold values from -0.1875 to 0.1875
- ffn_gain: bfloat16 [4096], replicated, may hold values from 0.099609375 to 1.8984375
- routing: int32 [256, 2], P('ep'), may hold values from 0 to 7, all different within a row; in each aligned block of 32 rows (0 to 31, 32 to 63, ...) at most 16 rows name the same one
- route_weight: float32 [256, 2], P('ep'), may hold values from 0.1 to 1
- expert_gate: bfloat16 [8, 4096, 2048], P('ep', None, 'tp'), may hold values from -0.25 to 0.25
- expert_up: bfloat16 [8, 4096, 2048], P('ep', None, 'tp'), may hold values from -0.25 to 0.25
- expert_down: bfloat16 [8, 2048, 4096], P('ep', 'tp'), may hold values from -0.03125 to 0.03125
Outputs:
- layer_out: bfloat16 [256, 4096], P('ep', 'tp')
- new_state: float32 [256, 8, 128, 128], P('ep', 'tp')
The draws below stay inside these ranges and needn't reach their ends.
Inputs may be any that keep to these rules, and one draw needn't show every extreme that they name: `routing`: each row names 2 different experts. In each aligned block of 32 rows (the rows of one device) no expert is named more than 16 times, a bound that some block reaches.
All inputs are finite; a program needn't handle non-finite values.
Results may differ from the reference program's by a relative error of at most 0.019.
Values may be sent and summed in bfloat16 or wider, within the bound.
A program may use at most 64 MiB of HBM per device.

```python
import math
import jax
import jax.numpy as jnp
import numpy as np
from jax import lax

D = 4096
HEADS = 8
HEAD = 128
FF = 2048
TOP_K = 2
B_DEV = 32
EXPERTS = 8
CAP = 16
TOKENS = 256
N_EP = 8
N_TP = 4


def shard_levels(stream_key, extent, pieces, smallest, high):
    factor_of = 1.0
    for dim, shards_of in pieces:
        heights = jax.random.uniform(jax.random.fold_in(jax.random.fold_in(stream_key, 6), dim), (shards_of,), jnp.float32, smallest / len(pieces), high / len(pieces))
        factor_of = factor_of * jnp.repeat(jnp.exp(heights), extent[dim] // shards_of).reshape((-1,) + (1,) * (len(extent) - 1 - dim))
    return factor_of


def shared_out(own_key, own, number, rows, count, top, limit, slope):
    sequence = jax.random.permutation(own_key, count)
    crowded, common = portions_of(count, rows * top, limit, slope, True), portions_of(count, rows * top, limit, slope, False)
    places = jnp.arange(count)

    def named(lengths, turn):
        used = int((lengths > 0).sum())
        fixed = max(1, used // 4)
        shifted = fixed + (places - fixed + turn * (used - fixed)) % max(1, count - fixed)
        return jnp.zeros((count,), jnp.int32).at[sequence[jnp.where(places < fixed, places, shifted)]].set(jnp.asarray(lengths, jnp.int32))

    lengths = jnp.where(number % 4 == 0, named(crowded, number // 4), named(common, number - number // 4 - 1))
    mixed = jax.random.permutation(jax.random.fold_in(own, 3), count)
    donor, taker = mixed[0:count // 2 * 2:2], mixed[1:count // 2 * 2:2]
    room = jnp.minimum(lengths[donor] - 1, limit - lengths[taker]) // 2
    room = jnp.where((donor == sequence[0]) | (taker == sequence[0]) | (lengths[taker] == 0), 0, jnp.maximum(room, 0))
    shifted = jax.random.randint(jax.random.fold_in(own, 4), (count // 2,), 0, 1 << 20) % (room + 1)
    lengths = lengths.at[donor].add(-shifted).at[taker].add(shifted)
    labels = jnp.searchsorted(jnp.cumsum(lengths), jnp.arange(rows * top), side="right").astype(jnp.int32)
    listing = labels.reshape(top, rows).T
    listing = listing[jax.random.permutation(jax.random.fold_in(own, 1), rows)]
    turn = jax.random.randint(jax.random.fold_in(own, 2), (rows, 1), 0, top)
    return jnp.take_along_axis(listing, (jnp.arange(top)[None, :] + turn) % top, axis=1)


def portions_of(amount, total, bound, slope, full):
    weights = [(1 << 20) // math.isqrt(standing ** slope) + 1 for standing in range(1, amount + 1)]
    largest = bound if full else min(bound, max(-(-total // amount), total * weights[0] // sum(weights)))
    least = 1 if total - largest >= amount - 1 else 0
    counts, rest = [largest] + [least] * (amount - 1), total - largest - least * (amount - 1)
    while rest > 0:
        candidates = [i for i in range(1, amount) if counts[i] < largest] or [i for i in range(1, amount) if counts[i] < bound]
        mass, remaining = sum([weights[i] for i in candidates]), rest
        for i in candidates:
            addition = min(bound - counts[i], max(1, remaining * weights[i] // mass), rest)
            counts[i] = counts[i] + addition
            rest = rest - addition
    return np.array(counts)


def scatter_about(key, extent, scale, bound, split=(), kind=jnp.bfloat16):
    array = scale * jax.random.normal(key, extent, jnp.float32)
    if split:
        array = array * shard_levels(key, extent, split, -0.22, 0.18)
    return jnp.clip(array, -bound, bound).astype(kind)


def setup_inputs(seed: int = 0) -> dict:
    streams_of = jax.random.split(jax.random.key(seed), 18)
    tokens = scatter_about(streams_of[0], (TOKENS, D), 1.0, 6.0, ((0, 8),))
    mix_gain = jnp.clip(1.0 + 0.18 * jax.random.normal(streams_of[1], (D,), jnp.float32), 0.099609375, 1.8984375).astype(jnp.bfloat16)
    query_weight = scatter_about(streams_of[2], (D, HEADS * HEAD), D ** -0.5, 0.09375, ((1, 4),))
    key_weight = scatter_about(streams_of[3], (D, HEADS * HEAD), D ** -0.5, 0.09375, ((1, 4),))
    value_weight = scatter_about(streams_of[4], (D, HEADS * HEAD), D ** -0.5, 0.09375, ((1, 4),))
    decay_weight = scatter_about(streams_of[5], (D, HEADS), D ** -0.5, 0.09375)
    strength_weight = scatter_about(streams_of[6], (D, HEADS), D ** -0.5, 0.09375)
    decay_rate = jnp.clip(jnp.exp(math.log(3.0) - 4.6051702 * jax.random.uniform(streams_of[7], (HEADS,), jnp.float32) ** shard_levels(streams_of[7], (HEADS,), ((0, 4),), -0.2, 0.2)), 0.03, 3.0)
    head_gain = jnp.clip(1.0 + 0.18 * jax.random.normal(streams_of[8], (HEAD,), jnp.float32), 0.099609375, 1.8984375).astype(jnp.bfloat16)
    memory_state = scatter_about(streams_of[9], (TOKENS, HEADS, HEAD, HEAD), 0.1, 0.6, ((0, 8), (1, 4)), jnp.float32)
    output_weight = scatter_about(streams_of[10], (HEADS * HEAD, D), (HEADS * HEAD) ** -0.5, 0.1875, ((0, 4),))
    ffn_gain = jnp.clip(1.0 + 0.18 * jax.random.normal(streams_of[11], (D,), jnp.float32), 0.099609375, 1.8984375).astype(jnp.bfloat16)
    routing_keys = jax.random.split(jax.random.fold_in(streams_of[12], 1), TOKENS // B_DEV)
    routing_turns = jax.random.permutation(jax.random.fold_in(streams_of[12], 3), TOKENS // B_DEV)
    routing = jax.vmap(lambda own, number: shared_out(jax.random.fold_in(streams_of[12], 2), own, number, B_DEV, EXPERTS, TOP_K, CAP, 2))(routing_keys, routing_turns).reshape((TOKENS, TOP_K))
    route_weight = jnp.clip(jnp.exp(math.log(1.0) - 2.3025851 * jax.random.uniform(streams_of[13], (TOKENS, TOP_K), jnp.float32) ** shard_levels(streams_of[13], (TOKENS, TOP_K), ((0, 8),), -0.2, 0.2)), 0.1, 1.0)
    expert_gate = scatter_about(streams_of[14], (EXPERTS, D, FF), (D // 9) ** -0.5, 0.25, ((0, 8), (2, 4)))
    expert_up = scatter_about(streams_of[15], (EXPERTS, D, FF), (D // 9) ** -0.5, 0.25, ((0, 8), (2, 4)))
    expert_down = scatter_about(streams_of[16], (EXPERTS, FF, D), (FF * 16) ** -0.5, 0.03125, ((0, 8), (1, 4)))
    return dict(tokens=tokens, mix_gain=mix_gain, query_weight=query_weight, key_weight=key_weight, value_weight=value_weight, decay_weight=decay_weight, strength_weight=strength_weight, decay_rate=decay_rate, head_gain=head_gain, memory_state=memory_state, output_weight=output_weight, ffn_gain=ffn_gain, routing=routing, route_weight=route_weight, expert_gate=expert_gate, expert_up=expert_up, expert_down=expert_down)


epsilon = 1e-06
clamp_limit = 7.0
swish_alpha = 1.702

def rms_scale(rows, gain):
    values = rows.astype(jnp.float32)
    scaled = values * lax.rsqrt(lax.optimization_barrier(jnp.mean(values * values, axis=-1, keepdims=True)) + epsilon)
    return (scaled * gain.astype(jnp.float32)).astype(jnp.bfloat16)

def round_keep(rounded):
    return lax.optimization_barrier(rounded).astype(jnp.float32)

def unit_rows(values):
    return values * lax.rsqrt(lax.optimization_barrier(jnp.sum(values * values, axis=-1, keepdims=True)) + epsilon)

def delta_step(projected, decay_log, strength, memory_state, head_gain):
    queries = unit_rows(jax.nn.silu(projected[:, 0])) * projected.shape[-1] ** (-0.5)
    keys_unit = unit_rows(jax.nn.silu(projected[:, 1]))
    values_new = jax.nn.silu(projected[:, 2])
    retained = memory_state * jnp.exp(decay_log)[:, :, None, None]
    recalled = jnp.einsum('thd,thde->the', keys_unit, retained, precision=lax.Precision.HIGHEST)
    corrected = strength[:, :, None] * (values_new - recalled)
    updated = retained + keys_unit[:, :, :, None] * corrected[:, :, None, :]
    readout = jnp.einsum('thd,thde->the', queries, updated, precision=lax.Precision.HIGHEST)
    scaled = readout * lax.rsqrt(lax.optimization_barrier(jnp.mean(readout * readout, axis=-1, keepdims=True)) + epsilon)
    mixed = scaled * head_gain.astype(jnp.float32)
    return (mixed.astype(jnp.bfloat16), updated)

def clamped_unit(gate_pre, up_pre):
    gate_cut = jnp.minimum(gate_pre, clamp_limit)
    up_cut = jnp.clip(up_pre, -clamp_limit, clamp_limit)
    return ((up_cut + 1.0) * gate_cut * jax.nn.sigmoid(swish_alpha * gate_cut)).astype(jnp.bfloat16)

def reference(tokens, mix_gain, query_weight, key_weight, value_weight, decay_weight, strength_weight, decay_rate, head_gain, memory_state, output_weight, ffn_gain, routing, route_weight, expert_gate, expert_up, expert_down):
    normed = rms_scale(tokens, mix_gain)
    joined = jnp.concatenate([query_weight, key_weight, value_weight], axis=1)
    projected = round_keep(jnp.dot(normed, joined, preferred_element_type=jnp.float32).astype(jnp.bfloat16))
    projected = projected.reshape(TOKENS, 3, HEADS, HEAD)
    decay_pre = jnp.dot(normed, decay_weight, preferred_element_type=jnp.float32)
    decay_log = -decay_rate[None, :] * jax.nn.softplus(decay_pre)
    strength = jax.nn.sigmoid(jnp.dot(normed, strength_weight, preferred_element_type=jnp.float32))
    mixed, new_state = delta_step(projected, decay_log, strength, memory_state, head_gain)
    mixed = mixed.reshape(TOKENS, HEADS * HEAD)
    shard_width = HEADS * HEAD // N_TP

    def add_shard(shard_id, running):
        offset = (shard_id * shard_width).astype(jnp.int32)
        rows_part = lax.dynamic_slice_in_dim(mixed, offset, shard_width, 1)
        weight_part = lax.dynamic_slice_in_dim(output_weight, offset, shard_width, 0)
        partial_term = jnp.dot(rows_part, weight_part, preferred_element_type=jnp.float32)
        return running + round_keep(partial_term.astype(jnp.bfloat16))
    mix_sum = lax.fori_loop(0, N_TP, add_shard, jnp.zeros((TOKENS, D), jnp.float32))
    residual = (tokens.astype(jnp.float32) + mix_sum).astype(jnp.bfloat16)
    ffn_in = rms_scale(residual, ffn_gain)
    pairs = B_DEV * TOP_K
    chosen = routing.reshape(N_EP, pairs)
    marks = (chosen[:, :, None] == jnp.arange(EXPERTS, dtype=jnp.int32)[None, None, :]).astype(jnp.int32)
    order_rank = lax.optimization_barrier(jnp.sum((jnp.cumsum(marks, axis=1) - 1) * marks, axis=2))
    block_id = jnp.arange(N_EP, dtype=jnp.int32)[:, None]
    position = (chosen * (N_EP * CAP) + block_id * CAP + order_rank).reshape(-1).astype(jnp.int32)
    owner = (block_id * B_DEV + jnp.arange(pairs, dtype=jnp.int32)[None, :] // TOP_K).reshape(-1).astype(jnp.int32)
    buffer = jnp.zeros((EXPERTS * N_EP * CAP, D), jnp.bfloat16).at[position].set(ffn_in[owner])
    buffer = buffer.reshape(EXPERTS, N_EP * CAP, D)
    ff_width = FF // N_TP

    def run_expert(expert_id):
        expert_rows = buffer[expert_id]
        gate_pre = jnp.dot(expert_rows, expert_gate[expert_id], preferred_element_type=jnp.float32)
        up_pre = jnp.dot(expert_rows, expert_up[expert_id], preferred_element_type=jnp.float32)
        hidden = clamped_unit(gate_pre, up_pre)
        down_rows = expert_down[expert_id]
        running = jnp.zeros((N_EP * CAP, D), jnp.float32)
        for shard_id in range(N_TP):
            partial_term = jnp.dot(hidden[:, shard_id * ff_width:(shard_id + 1) * ff_width], down_rows[shard_id * ff_width:(shard_id + 1) * ff_width], preferred_element_type=jnp.float32)
            running = running + round_keep(partial_term.astype(jnp.bfloat16))
        return running.astype(jnp.bfloat16)
    outputs = lax.map(run_expert, jnp.arange(EXPERTS, dtype=jnp.int32)).reshape(EXPERTS * N_EP * CAP, D)
    picked = outputs[position].astype(jnp.float32).reshape(TOKENS, TOP_K, D)
    routed = lax.optimization_barrier(jnp.sum(picked * route_weight[:, :, None], axis=1))
    layer_out = (residual.astype(jnp.float32) + routed).astype(jnp.bfloat16)
    return (layer_out, new_state)
```

```python
import functools

import jax
import jax.numpy as jnp
from jax import lax
from jax.experimental import pallas as pl
from jax.experimental.pallas import tpu as pltpu
from jax.sharding import PartitionSpec as P

epsilon = 1e-06
clamp_limit = 7.0
swish_alpha = 1.702
MESH = pl.DeviceIdType.MESH
TOKEN_BLOCK = 8
MIX_VMEM = 20 * 1024 * 1024
EXPERT_VMEM = 32 * 1024 * 1024


def silu(values):
    return values * jax.nn.sigmoid(values)


def mix_kernel(
    tok_hbm, gain_hbm, dw_hbm, sw_hbm, rate_hbm, hg_hbm, wq_hbm, wk_hbm, wv_hbm, state_hbm,
    mixed_ref, new_hbm, tok_ref, gain_ref, dw_ref, sw_ref, rate_ref, hg_ref, wq_ref, wk_ref,
    wv_ref, state, q_scr, k_scr, v_scr, dec_scr, str_scr, ro_scr, l_sem, in_sem, out_sem,
):
    heads = state.shape[1]
    width = state.shape[2]
    block = TOKEN_BLOCK
    steps = state.shape[0] // block
    loads = []
    for i, (src, dst) in enumerate((
        (tok_hbm, tok_ref), (gain_hbm, gain_ref), (wq_hbm, wq_ref), (dw_hbm, dw_ref),
        (sw_hbm, sw_ref), (rate_hbm, rate_ref), (hg_hbm, hg_ref), (wk_hbm, wk_ref),
        (wv_hbm, wv_ref),
    )):
        loads.append(pltpu.make_async_copy(src, dst, l_sem.at[i]))
        loads[-1].start()
    tok_in, gain_in, wq_in, dw_in, sw_in, rate_in, hg_in, wk_in, wv_in = loads

    def take(i):
        rows = pl.ds(pl.multiple_of(i * block, block), block)
        return pltpu.make_async_copy(state_hbm.at[rows], state.at[rows], in_sem.at[i])

    def give(i):
        rows = pl.ds(pl.multiple_of(i * block, block), block)
        return pltpu.make_async_copy(state.at[rows], new_hbm.at[rows], out_sem.at[i])

    for i in range(steps):
        take(i).start()
    head_start = lax.axis_index("tp") * heads

    tok_in.wait()
    gain_in.wait()
    values = tok_ref[...].astype(jnp.float32)
    scale = lax.rsqrt(jnp.mean(values * values, axis=-1, keepdims=True) + epsilon)
    gain = gain_ref[...].astype(jnp.float32)
    lanes = gain.shape[1]
    normed = jnp.concatenate(
        [
            (values[:, i * lanes:(i + 1) * lanes] * scale * gain[i:i + 1]).astype(jnp.bfloat16)
            for i in range(gain.shape[0])
        ],
        axis=1,
    )

    def project(copy, w_ref):
        copy.wait()
        out = jnp.dot(normed, w_ref[...], preferred_element_type=jnp.float32)
        return silu(out.astype(jnp.bfloat16).astype(jnp.float32))

    dw_in.wait()
    sw_in.wait()
    rate_in.wait()
    wide = normed.astype(jnp.float32)

    def per_head(w_ref, h):
        w = w_ref[...].astype(jnp.float32)
        mine = lax.broadcasted_iota(jnp.int32, w.shape, 0) == head_start + h
        row = jnp.sum(jnp.where(mine, w, 0.0), axis=0, keepdims=True)
        return jnp.sum(wide * row, axis=1, keepdims=True)

    for h in range(heads):
        part = slice(h * width, (h + 1) * width)
        d_h, s_h = per_head(dw_ref, h), per_head(sw_ref, h)
        soft = jnp.maximum(d_h, 0.0) + jnp.log1p(jnp.exp(-jnp.abs(d_h)))
        decay = jnp.exp(-rate_ref[:, h:h + 1] * soft)
        spread = (d_h.shape[0], width)
        dec_scr[:, part] = jnp.broadcast_to(decay, spread)
        str_scr[:, part] = jnp.broadcast_to(jax.nn.sigmoid(s_h), spread)

    def unit(values):
        return values * lax.rsqrt(jnp.sum(values * values, axis=-1, keepdims=True) + epsilon)

    queries = project(wq_in, wq_ref)
    for h in range(heads):
        part = slice(h * width, (h + 1) * width)
        q_scr[:, part] = unit(queries[:, part]) * width ** (-0.5)
    keys = project(wk_in, wk_ref)
    for h in range(heads):
        part = slice(h * width, (h + 1) * width)
        k_scr[:, part] = unit(keys[:, part])
    v_scr[...] = project(wv_in, wv_ref)

    def advance(step, carry):
        take(step).wait()
        rows = pl.ds(pl.multiple_of(step * block, block), block)
        for h in range(heads):
            part = slice(h * width, (h + 1) * width)
            q8, k8, v8 = q_scr[rows, part], k_scr[rows, part], v_scr[rows, part]
            d8, s8 = dec_scr[rows, part], str_scr[rows, part]
            qk8 = jnp.sum(q8 * k8, axis=1, keepdims=True)
            q_t, k_t = jnp.transpose(q8), jnp.transpose(k8)
            outs = []
            for t in range(block):
                memory = state[step * block + t, h]
                k_col, q_col = k_t[:, t:t + 1], q_t[:, t:t + 1]
                k_m = jnp.sum(memory * k_col, axis=0, keepdims=True)
                q_m = jnp.sum(memory * q_col, axis=0, keepdims=True)
                d_t = d8[t:t + 1]
                corrected = s8[t:t + 1] * (v8[t:t + 1] - d_t * k_m)
                state[step * block + t, h] = memory * d_t + k_col * corrected
                outs.append(d_t * q_m + qk8[t:t + 1] * corrected)
            ro_scr[rows, part] = jnp.concatenate(outs, axis=0)
        give(step).start()
        return carry

    lax.fori_loop(0, steps, advance, 0)

    hg_in.wait()
    head_gain = hg_ref[...].astype(jnp.float32)
    for h in range(heads):
        part = slice(h * width, (h + 1) * width)
        read = ro_scr[:, part]
        scale = lax.rsqrt(jnp.mean(read * read, axis=-1, keepdims=True) + epsilon)
        mixed_ref[:, part] = (read * scale * head_gain).astype(jnp.bfloat16)
    for i in range(steps):
        give(i).wait()


def mix_step(tokens, mix_gain, wq, wk, wv, dw, sw, rate, head_gain, state):
    rows, _ = tokens.shape
    heads, width = state.shape[1], state.shape[2]
    inner = heads * width
    hbm = pl.BlockSpec(memory_space=pltpu.HBM)
    sem = pltpu.SemaphoreType.DMA
    steps = rows // TOKEN_BLOCK
    args = [
        pltpu.with_memory_space_constraint(a, pltpu.HBM) if a.size > 1 else a
        for a in (tokens, mix_gain, dw, sw, rate, head_gain, wq, wk, wv, state)
    ]
    return pl.pallas_call(
        mix_kernel,
        out_shape=(
            jax.ShapeDtypeStruct((rows, inner), jnp.bfloat16),
            jax.ShapeDtypeStruct(state.shape, state.dtype),
        ),
        in_specs=[hbm] * 10,
        out_specs=(pl.BlockSpec(memory_space=pltpu.VMEM), hbm),
        scratch_shapes=[pltpu.VMEM(a.shape, a.dtype) for a in args]
        + [pltpu.VMEM((rows, inner), jnp.float32)] * 6
        + [sem((9,)), sem((steps,)), sem((steps,))],
        compiler_params=pltpu.CompilerParams(vmem_limit_bytes=MIX_VMEM),
        name="mix",
    )(*args)


def expert_kernel(
    groups, tp_width, capacity,
    mixed_ref, tok_ref, gain_ref, route_ref, weight_ref, wo, wg_hbm, wu_hbm, wd_hbm,
    out_ref,
    wg, wu, wd, gain_scr,
    part, rs_in, ss_out, ss_in, sc_out, sc_in, out_buf, x_buf, po, pair_in, pair_sum, y_in,
    ret_out, ret_in, res_scr, gate_acc, up_acc,
    load_sem, rs_s, rs_r, ss_s, ss_r, sc_s, sc_r, a2a_s, a2a_r, agy_s, agy_r, agp_s, agp_r,
    pr_s, pr_r, yr_s, yr_r, rt_s, rt_r,
):
    ep, tp = lax.axis_index("ep"), lax.axis_index("tp")
    rows, model = tok_ref.shape
    share = model // tp_width
    chips = tp_width // 2
    slots = groups * capacity
    chip, core = tp // 2, lax.rem(tp, 2)
    partner = chip * 2 + 1 - core
    cols = pl.ds(pl.multiple_of(tp * share, share), share)

    loads = [
        pltpu.make_async_copy(src, dst, load_sem.at[i])
        for i, (src, dst) in enumerate(((wg_hbm, wg), (wu_hbm, wu), (wd_hbm, wd)))
    ]
    wg_in, wu_in, wd_in = loads
    for copy in loads:
        copy.start()

    barrier = pltpu.get_barrier_semaphore()
    for k in range(1, groups):
        pl.semaphore_signal(
            barrier, inc=1, device_id=(lax.rem(ep + k, groups), tp), device_id_type=MESH
        )
    for k in range(1, tp_width):
        pl.semaphore_signal(
            barrier, inc=1, device_id=(ep, lax.rem(tp + k, tp_width)), device_id_type=MESH
        )

    sends = []

    def send(src, dst, s_sem, r_sem, target):
        copy = pltpu.make_async_remote_copy(
            src_ref=src, dst_ref=dst, send_sem=s_sem, recv_sem=r_sem,
            device_id=target, device_id_type=MESH,
        )
        copy.start()
        sends.append(copy)

    def arrive(ref, r_sem, s_sem):
        pltpu.make_async_remote_copy(
            src_ref=ref, dst_ref=ref, send_sem=s_sem, recv_sem=r_sem,
            device_id=(ep, partner), device_id_type=MESH,
        ).wait_recv()

    peers = []
    for c in list(range(1, chips)) + [0]:
        for b in (0, 1):
            if c or b:
                at = lax.rem(chip + c, chips) * 2
                peers.append((c * 2 + b, at + (1 - core if b else core)))

    def project(p):
        lanes = pl.ds(pl.multiple_of(p * share, share), share)
        part[p] = jnp.dot(
            mixed_ref[...], wo[:, lanes], preferred_element_type=jnp.float32
        ).astype(jnp.bfloat16)

    for _, to in peers[:-1]:
        project(to)
    pl.semaphore_wait(barrier, tp_width - 1 + groups - 1)
    for j, to in peers:
        if j == 1:
            project(to)
        send(part.at[to], rs_in.at[j], rs_s.at[j], rs_r.at[j], (ep, to))
    project(tp)

    top = route_ref.shape[0]
    slot_ids = lax.broadcasted_iota(jnp.int32, (slots, rows), 0)
    slot_expert = slot_ids // capacity
    slot_rank = slot_ids % capacity
    marks = [route_ref[k:k + 1, :] == slot_expert for k in range(top)]
    named = functools.reduce(lambda a, b: a + b, [m.astype(jnp.float32) for m in marks])
    before = (
        lax.broadcasted_iota(jnp.int32, (rows, rows), 0)
        < lax.broadcasted_iota(jnp.int32, (rows, rows), 1)
    ).astype(jnp.float32).astype(jnp.bfloat16)
    ranks = jnp.dot(named.astype(jnp.bfloat16), before, preferred_element_type=jnp.float32)
    here = ranks == slot_rank.astype(jnp.float32)
    chosen = [jnp.where(jnp.logical_and(m, here), 1.0, 0.0) for m in marks]
    place = functools.reduce(lambda a, b: a + b, chosen)
    place_t = jnp.transpose(place)
    place = place.astype(jnp.bfloat16)
    blend = functools.reduce(
        lambda a, b: a + b, [c * weight_ref[k:k + 1, :] for k, c in enumerate(chosen)]
    )
    gain_scr[...] = gain_ref[...].astype(jnp.float32)
    diag = (
        lax.broadcasted_iota(jnp.int32, (rows, 128), 0)
        == lax.broadcasted_iota(jnp.int32, (rows, 128), 1)
    )

    total = tok_ref[:, cols].astype(jnp.float32)
    mix_sum = part[tp].astype(jnp.float32)
    for j, _ in reversed(peers):
        arrive(rs_in.at[j], rs_r.at[j], rs_s.at[j])
        mix_sum = mix_sum + rs_in[j].astype(jnp.float32)
    residual = (total + mix_sum).astype(jnp.bfloat16)
    res_scr[...] = residual
    res = residual.astype(jnp.float32)
    blocks = share // 128
    scaled = jnp.concatenate(
        [
            (
                res[:, i * 128:(i + 1) * 128] * gain_scr[pl.ds(tp * blocks + i, 1), :]
            ).astype(jnp.bfloat16)
            for i in range(blocks)
        ],
        axis=1,
    )
    outgoing = jnp.dot(place, scaled, preferred_element_type=jnp.float32).astype(jnp.bfloat16)
    out_buf[...] = outgoing.reshape(groups, capacity, share)
    for k in range(1, groups):
        to = lax.rem(ep + k, groups)
        send(out_buf.at[to], x_buf.at[tp, ep], a2a_s.at[k], a2a_r.at[k], (to, tp))
    x_buf[tp, ep] = out_buf[ep]

    squares = jnp.sum(res * res, axis=-1, keepdims=True)
    ss_out[...] = jnp.sum(jnp.where(diag, squares, 0.0), axis=0, keepdims=True)
    for j, to in peers:
        send(ss_out, ss_in.at[j], ss_s.at[j], ss_r.at[j], (ep, to))

    for k in range(groups):
        src = lax.rem(ep + groups - k, groups)
        block = x_buf.at[tp, src]
        if k > 0:
            arrive(block, a2a_r.at[k], a2a_s.at[k])
        for c in range(1, chips):
            to = lax.rem(chip + c, chips) * 2 + core
            send(block, block, agy_s.at[c, k], agy_r.at[c, k], (ep, to))
        send(block, block, agp_s.at[0, k], agp_r.at[0, k], (ep, partner))

    sum_row = ss_out[...]
    for j, _ in peers:
        arrive(ss_in.at[j], ss_r.at[j], ss_s.at[j])
        sum_row = sum_row + ss_in[j]
    scale_row = lax.rsqrt(sum_row / model + epsilon)
    scale = jnp.sum(jnp.where(diag, scale_row, 0.0), axis=1, keepdims=True)
    slot_scale = jnp.sum(place_t * scale, axis=0, keepdims=True)
    sc_out[...] = slot_scale
    for k in range(1, groups):
        to = lax.rem(ep + k, groups)
        send(sc_out, sc_in.at[ep], sc_s.at[k], sc_r.at[k], (to, tp))
    sc_in[ep] = slot_scale

    wg_in.wait()
    wu_in.wait()

    def accumulate(j, first):
        x = x_buf[j].reshape(slots, share)
        depth = pl.ds(pl.multiple_of(j * share, share), share)
        g = jnp.dot(x, wg[depth, :], preferred_element_type=jnp.float32)
        u = jnp.dot(x, wu[depth, :], preferred_element_type=jnp.float32)
        gate_acc[...] = g if first else gate_acc[...] + g
        up_acc[...] = u if first else up_acc[...] + u

    accumulate(tp, True)
    for c in range(1, chips):
        origin = lax.rem(chip + chips - c, chips) * 2 + core
        for k in range(groups):
            src = lax.rem(ep + groups - k, groups)
            block = x_buf.at[origin, src]
            arrive(block, agy_r.at[c, k], agy_s.at[c, k])
            send(block, block, agp_s.at[c, k], agp_r.at[c, k], (ep, partner))
    for k in range(groups):
        src = lax.rem(ep + groups - k, groups)
        arrive(x_buf.at[partner, src], agp_r.at[0, k], agp_s.at[0, k])
    accumulate(partner, False)
    for c in range(1, chips):
        other = lax.rem(chip + chips - c, chips) * 2
        accumulate(other + core, False)
        for k in range(groups):
            src = lax.rem(ep + groups - k, groups)
            arrive(x_buf.at[other + 1 - core, src], agp_r.at[c, k], agp_s.at[c, k])
        accumulate(other + 1 - core, False)

    for k in range(1, groups):
        src = lax.rem(ep + groups - k, groups)
        arrive(sc_in.at[src], sc_r.at[k], sc_s.at[k])
    picks = (
        lax.broadcasted_iota(jnp.int32, (capacity, slots), 1)
        == lax.broadcasted_iota(jnp.int32, (capacity, slots), 0) + ep * capacity
    )
    row_scale = jnp.concatenate(
        [
            jnp.sum(jnp.where(picks, sc_in[s], 0.0), axis=1, keepdims=True)
            for s in range(groups)
        ],
        axis=0,
    )
    gate_cut = jnp.minimum(gate_acc[...] * row_scale, clamp_limit)
    up_cut = jnp.clip(up_acc[...] * row_scale, -clamp_limit, clamp_limit)
    hidden = ((up_cut + 1.0) * gate_cut * jax.nn.sigmoid(swish_alpha * gate_cut)).astype(
        jnp.bfloat16
    )

    wd_in.wait()

    def down(p):
        lanes = pl.ds(pl.multiple_of(p * share, share), share)
        term = jnp.dot(hidden, wd[:, lanes], preferred_element_type=jnp.float32)
        po[p] = term.astype(jnp.bfloat16).reshape(groups, capacity, share)

    order = [lax.rem(chip + c, chips) for c in list(range(1, chips)) + [0]]
    for i, c in enumerate(order):
        down(c * 2 + 1 - core)
        send(po.at[c * 2 + 1 - core], pair_in.at[i], pr_s.at[i], pr_r.at[i], (ep, partner))
        if i < chips - 1:
            down(c * 2 + core)
    for i, c in enumerate(order[:-1]):
        arrive(pair_in.at[i], pr_r.at[i], pr_s.at[i])
        for k in list(range(1, groups)) + [0]:
            s = lax.rem(ep + k, groups)
            pair_sum[i, s] = (
                po[c * 2 + core, s].astype(jnp.float32) + pair_in[i, s].astype(jnp.float32)
            ).astype(jnp.bfloat16)
            send(
                pair_sum.at[i, s], y_in.at[i, s], yr_s.at[i, k], yr_r.at[i, k],
                (ep, c * 2 + core),
            )
    last = chips - 1
    down(tp)
    arrive(pair_in.at[last], pr_r.at[last], pr_s.at[last])
    for k in list(range(1, groups)) + [0]:
        s = lax.rem(ep + k, groups)
        term = po[tp, s].astype(jnp.float32) + pair_in[last, s].astype(jnp.float32)
        for i in range(chips - 1):
            arrive(y_in.at[i, s], yr_r.at[i, k], yr_s.at[i, k])
            term = term + y_in[i, s].astype(jnp.float32)
        if k > 0:
            ret_out[s] = term.astype(jnp.bfloat16)
            send(ret_out.at[s], ret_in.at[ep], rt_s.at[k], rt_r.at[k], (s, tp))
        else:
            ret_in[s] = term.astype(jnp.bfloat16)
    for k in range(1, groups):
        src = lax.rem(ep + groups - k, groups)
        arrive(ret_in.at[src], rt_r.at[k], rt_s.at[k])

    back = ret_in[...].reshape(slots, share)
    high = blend.astype(jnp.bfloat16)
    low = (blend - high.astype(jnp.float32)).astype(jnp.bfloat16)
    dims = (((0,), (0,)), ((), ()))
    routed = lax.dot_general(high, back, dims, preferred_element_type=jnp.float32)
    routed = routed + lax.dot_general(low, back, dims, preferred_element_type=jnp.float32)
    out_ref[...] = (res_scr[...].astype(jnp.float32) + routed).astype(jnp.bfloat16)
    for copy in sends:
        copy.wait_send()


def expert_step(tokens, mixed, gain, routing, route_weight, wo, wg, wu, wd):
    groups, tp_width = lax.axis_size("ep"), lax.axis_size("tp")
    rows, model = tokens.shape
    share = model // tp_width
    chips = tp_width // 2
    need = 2 * rows * routing.shape[0] // groups
    capacity = -(-need // 16) * 16
    slots = groups * capacity
    ff = wg.shape[1]
    bf16, f32 = jnp.bfloat16, jnp.float32
    wg, wu, wd = [pltpu.with_memory_space_constraint(a, pltpu.HBM) for a in (wg, wu, wd)]
    vmem = pl.BlockSpec(memory_space=pltpu.VMEM)
    hbm = pl.BlockSpec(memory_space=pltpu.HBM)
    block = (groups, capacity, share)
    sem = pltpu.SemaphoreType.DMA
    return pl.pallas_call(
        functools.partial(expert_kernel, groups, tp_width, capacity),
        out_shape=jax.ShapeDtypeStruct((rows, share), bf16),
        in_specs=[vmem] * 6 + [hbm] * 3,
        out_specs=vmem,
        scratch_shapes=[
            pltpu.VMEM(wg.shape, bf16),
            pltpu.VMEM(wu.shape, bf16), pltpu.VMEM(wd.shape, bf16),
            pltpu.VMEM(gain.shape, f32),
            pltpu.VMEM((tp_width, rows, share), bf16),
            pltpu.VMEM((tp_width, rows, share), bf16),
            pltpu.VMEM((1, 128), f32),
            pltpu.VMEM((tp_width, 1, 128), f32),
            pltpu.VMEM((1, slots), f32),
            pltpu.VMEM((groups, 1, slots), f32),
            pltpu.VMEM(block, bf16),
            pltpu.VMEM((tp_width,) + block, bf16),
            pltpu.VMEM((tp_width,) + block, bf16),
            pltpu.VMEM((chips,) + block, bf16),
            pltpu.VMEM((chips,) + block, bf16),
            pltpu.VMEM((chips,) + block, bf16),
            pltpu.VMEM(block, bf16),
            pltpu.VMEM(block, bf16),
            pltpu.VMEM((rows, share), bf16),
            pltpu.VMEM((slots, ff), f32),
            pltpu.VMEM((slots, ff), f32),
            sem((3,)),
            sem((tp_width,)), sem((tp_width,)),
            sem((tp_width,)), sem((tp_width,)),
            sem((groups,)), sem((groups,)),
            sem((groups,)), sem((groups,)),
            sem((chips, groups)), sem((chips, groups)),
            sem((chips, groups)), sem((chips, groups)),
            sem((chips,)), sem((chips,)),
            sem((chips, groups)), sem((chips, groups)),
            sem((groups,)), sem((groups,)),
        ],
        compiler_params=pltpu.CompilerParams(
            collective_id=0, has_side_effects=True, vmem_limit_bytes=EXPERT_VMEM
        ),
        name="experts",
    )(mixed, tokens, gain, routing, route_weight, wo, wg, wu, wd)


def on_device(
    tokens,
    mix_gain,
    query_weight,
    key_weight,
    value_weight,
    decay_weight,
    strength_weight,
    decay_rate,
    head_gain,
    memory_state,
    output_weight,
    ffn_gain,
    routing,
    route_weight,
    expert_gate,
    expert_up,
    expert_down,
):
    mixed, new_state = mix_step(
        tokens, mix_gain.reshape(-1, 128), query_weight, key_weight, value_weight,
        decay_weight.T, strength_weight.T, decay_rate[None, :], head_gain[None, :], memory_state,
    )
    layer_out = expert_step(
        tokens, mixed, ffn_gain.reshape(-1, 128), routing.T, route_weight.T, output_weight,
        expert_gate[0], expert_up[0], expert_down[0],
    )
    return (layer_out, new_state)


def solution(mesh):
    placed = (
        P("ep", None),
        P(),
        P(None, "tp"),
        P(None, "tp"),
        P(None, "tp"),
        P(),
        P(),
        P("tp"),
        P(),
        P("ep", "tp", None, None),
        P("tp", None),
        P(),
        P("ep", None),
        P("ep", None),
        P("ep", None, "tp"),
        P("ep", None, "tp"),
        P("ep", "tp", None),
    )
    return jax.shard_map(
        on_device,
        mesh=mesh,
        in_specs=placed,
        out_specs=(P("ep", "tp"), P("ep", "tp", None, None)),
        check_vma=False,
    )
```
